32 devices in a mesh: sp: 4 (over z), fs: 4 (over y, x), tp: 2 (over core).
Axes of the slice: x: 2, y: 2, z: 4, core: 2. Of those that a mesh axis runs over, the one named last changes fastest.
Arguments:
- activations: bfloat16 [4, 1024, 4096], P('fs', 'sp'), may hold values from -60 to 60
- input_norm_gain: float32 [4096], replicated, may hold values from 0.1 to 1.9
- pooling_channel_weight: bfloat16 [4096, 1024], P(('sp', 'fs'), 'tp'), may hold values from -0.09375 to 0.09375
- query_projection_weight: bfloat16 [4096, 1024], P(('sp', 'fs'), 'tp'), may hold values from -0.09375 to 0.09375
- key_projection_weight: bfloat16 [4096, 1024], P(('sp', 'fs'), 'tp'), may hold values from -0.09375 to 0.09375
- value_projection_weight: bfloat16 [4096, 1024], P(('sp', 'fs'), 'tp'), may hold values from -0.09375 to 0.09375
- output_gate_weight: bfloat16 [4096, 1024], P(('sp', 'fs'), 'tp'), may hold values from -0.09375 to 0.09375
- decay_first_factor: bfloat16 [4096, 64], P(('sp', 'fs')), may hold values from -0.09375 to 0.09375
- decay_second_factor: bfloat16 [64, 1024], P(None, 'tp'), may hold values from -0.75 to 0.75
- decay_gate_bias: float32 [1024], P('tp')
- decay_extra_log: float32 [16, 1024], P('tp', 'sp'), may hold values from -1.5 to 0
- head_norm_gain: float32 [1024], P('tp'), may hold values from 0.1 to 1.9
- starting_state: float32 [4, 16, 64, 64], P('fs', 'tp'), may hold values from -192 to 192
- pooling_group_weight: bfloat16 [8, 128, 128], P('tp'), may hold values from -0.5 to 0.5
- pooling_channel_scale: float32 [1024], P('tp'), may hold values from 0.1 to 1.9
- pooling_output_rows: bfloat16 [1024, 4096], P('sp', 'tp'), may hold values from -0.125 to 0.125
- attention_output_rows: bfloat16 [1024, 4096], P('sp', 'tp'), may hold values from -0.125 to 0.125
Outputs:
- mixed: bfloat16 [4, 1024, 4096], P('fs', 'sp', 'tp')
The draws below stay inside these ranges and needn't reach their ends.
All inputs are finite; a program needn't handle non-finite values.
Results may differ from the reference program's by a relative error of at most 0.012.
Values may be sent and summed in bfloat16 or wider, within the bound.
A program may use at most 128 MiB of HBM per device.

```python
import math
import jax
import jax.numpy as jnp
from jax import lax

D = 4096
POOL_WIDTH = 1024
POOL_GROUP_WIDTH = 128
GLA_HEADS = 16
HEAD_WIDTH = 64
RANK = 64
BLOCK = 64
REACH = 15
TOK_DEV = 256
LENGTH = 1024
SEQS = 4
POOL_GROUPS = 8
GLA_WIDTH = 1024


def draw_activations(key, part):
    normal_part = jax.random.normal(jax.random.fold_in(key, 1), (SEQS, LENGTH, D), jnp.float32)
    drawn = jnp.clip(normal_part, -6.0, 6.0)
    return drawn.astype(jnp.bfloat16)


def draw_decay_gate_bias(key, part):
    slow_share = 0.5
    slow_heads = jax.random.bernoulli(jax.random.fold_in(key, 11), slow_share, (GLA_HEADS,))
    jitter = jax.random.uniform(jax.random.fold_in(key, 12), (GLA_HEADS, HEAD_WIDTH), jnp.float32, -0.3, 0.3)
    slow_level = math.log(LENGTH / (0.3 * 16.0))
    levels = jnp.where(slow_heads[:, None], slow_level, 0.7) + jitter
    return levels.reshape(GLA_HEADS * HEAD_WIDTH).astype(jnp.float32)


def draw_decay_extra_log(key, part):
    shard_count = LENGTH // TOK_DEV
    rates = jnp.exp(jax.random.uniform(jax.random.fold_in(key, 21), (shard_count,), jnp.float32, math.log(0.15), math.log(1.2)))
    baseline = -jnp.repeat(rates, TOK_DEV) / LENGTH
    spots = jax.random.randint(jax.random.fold_in(key, 22), (GLA_HEADS, 2), 0, LENGTH)
    depths = jnp.log(jax.random.uniform(jax.random.fold_in(key, 23), (GLA_HEADS, 2), jnp.float32, 0.5, 0.8))
    hits = (jnp.arange(LENGTH)[None, None, :] == spots[:, :, None]).astype(jnp.float32) * depths[:, :, None]
    return (baseline[None, :] + jnp.sum(hits, axis=1)).astype(jnp.float32)


def level_of(key, shape, pieces, low, largest):
    loudness, own = 1.0, jax.random.fold_in(key, 6)
    for dim, blocks in pieces:
        steps = jnp.exp(jax.random.uniform(jax.random.fold_in(own, dim), (blocks,), jnp.float32, low / len(pieces), largest / len(pieces)))
        loudness = loudness * jnp.repeat(steps, shape[dim] // blocks).reshape([-1 if axis == dim else 1 for axis in range(len(shape))])
    return loudness


def gaussian(key, extent, width, reach, shards=(), kind=jnp.bfloat16):
    entries = width * jax.random.normal(key, extent, jnp.float32)
    if shards:
        entries = entries * level_of(key, extent, shards, -0.22, 0.18)
    return jnp.clip(entries, -reach, reach).astype(kind)


def setup_inputs(seed: int = 0) -> dict:
    streams_of = jax.random.split(jax.random.key(seed), 18)
    return {
        "activations": draw_activations(jax.random.fold_in(streams_of[17], 71), 0),
        "input_norm_gain": jnp.clip(1.0 + 0.18 * jax.random.normal(streams_of[1], (D,), jnp.float32), 0.1, 1.9),
        "pooling_channel_weight": gaussian(streams_of[2], (D, POOL_WIDTH), D ** -0.5, 0.09375, ((0, 16), (1, 2))),
        "query_projection_weight": gaussian(streams_of[3], (D, GLA_WIDTH), D ** -0.5, 0.09375, ((0, 16), (1, 2))),
        "key_projection_weight": gaussian(streams_of[4], (D, GLA_WIDTH), D ** -0.5, 0.09375, ((0, 16), (1, 2))),
        "value_projection_weight": gaussian(streams_of[5], (D, GLA_WIDTH), D ** -0.5, 0.09375, ((0, 16), (1, 2))),
        "output_gate_weight": gaussian(streams_of[6], (D, GLA_WIDTH), D ** -0.5, 0.09375, ((0, 16), (1, 2))),
        "decay_first_factor": gaussian(streams_of[7], (D, RANK), D ** -0.5, 0.09375, ((0, 16),)),
        "decay_second_factor": gaussian(streams_of[8], (RANK, GLA_WIDTH), RANK ** -0.5, 0.75, ((1, 2),)),
        "decay_gate_bias": draw_decay_gate_bias(jax.random.fold_in(streams_of[17], 71), 0),
        "decay_extra_log": draw_decay_extra_log(jax.random.fold_in(streams_of[17], 71), 0),
        "head_norm_gain": jnp.clip(1.0 + 0.18 * jax.random.normal(streams_of[11], (GLA_WIDTH,), jnp.float32), 0.1, 1.9),
        "starting_state": gaussian(streams_of[12], (SEQS, GLA_HEADS, HEAD_WIDTH, HEAD_WIDTH), (LENGTH ** 0.5), 192.0, ((0, 4), (1, 2)), jnp.float32),
        "pooling_group_weight": gaussian(streams_of[13], (POOL_GROUPS, POOL_GROUP_WIDTH, POOL_GROUP_WIDTH), POOL_GROUP_WIDTH ** -0.5, 0.5, ((0, 2),)),
        "pooling_channel_scale": jnp.clip(1.0 + 0.18 * jax.random.normal(streams_of[14], (POOL_WIDTH,), jnp.float32), 0.1, 1.9),
        "pooling_output_rows": gaussian(streams_of[15], (POOL_WIDTH, D), (POOL_WIDTH + GLA_WIDTH) ** -0.5, 0.125, ((0, 4), (1, 2))),
        "attention_output_rows": gaussian(streams_of[16], (GLA_WIDTH, D), (POOL_WIDTH + GLA_WIDTH) ** -0.5, 0.125, ((0, 4), (1, 2))),
    }


norm_eps = 1e-06
decay_temper = 16.0
highest = lax.Precision.HIGHEST

def window_levels(extended, total_row_count):
    width_two = extended[:, 1:] + extended[:, :-1]
    width_four = width_two[:, 2:] + width_two[:, :-2]
    width_eight = width_four[:, 4:] + width_four[:, :-4]
    width_sixteen = width_eight[:, 8:] + width_eight[:, :-8]
    return (width_two[:, -total_row_count:], width_four[:, -total_row_count:], width_eight[:, -total_row_count:], width_sixteen)

def pool_reference(pool_input, pooling_group_weight, pooling_channel_scale):
    sequence_count, length_all, channels = pool_input.shape
    current = pool_input.astype(jnp.float32)
    extended = jnp.concatenate([jnp.zeros((sequence_count, REACH, channels), jnp.float32), current], axis=1)
    window_sums = window_levels(extended, length_all)
    level_ids = jnp.arange(channels) // POOL_GROUP_WIDTH % 4
    window = jnp.where(level_ids == 0, 2.0, jnp.where(level_ids == 1, 4.0, jnp.where(level_ids == 2, 8.0, 16.0))).astype(jnp.float32)
    chosen = jnp.where(level_ids == 0, window_sums[0], jnp.where(level_ids == 1, window_sums[1], jnp.where(level_ids == 2, window_sums[2], window_sums[3])))
    positions = jnp.arange(length_all).astype(jnp.float32)
    counts = jnp.minimum(positions[:, None] + 1.0, window[None, :])
    deviation = (chosen / counts - current).astype(jnp.bfloat16)
    grouped = deviation.reshape(sequence_count, length_all, POOL_GROUPS, POOL_GROUP_WIDTH).astype(jnp.float32)
    mixture = jnp.einsum('btgc,gcd->btgd', grouped, pooling_group_weight.astype(jnp.float32))
    return (mixture.reshape(sequence_count, length_all, channels) * pooling_channel_scale).astype(jnp.bfloat16)

def decay_log_values(decay_lower_bound, decay_second_factor, decay_gate_bias, decay_extra_log):
    sequence_count, total_row_count, rank_width = decay_lower_bound.shape
    gate_input = jnp.dot(decay_lower_bound.reshape(sequence_count * total_row_count, rank_width), decay_second_factor, preferred_element_type=jnp.float32) + decay_gate_bias
    logarithm_rates = jax.nn.log_sigmoid(gate_input) / decay_temper
    local_head_count = decay_extra_log.shape[0]
    logarithm_rates = logarithm_rates.reshape(sequence_count, total_row_count, local_head_count, HEAD_WIDTH) + decay_extra_log.T[None, :, :, None]
    return logarithm_rates.reshape(sequence_count, total_row_count, local_head_count * HEAD_WIDTH)

def to_blocks(source, local_head_count):
    sequence_count, total_row_count, _ = source.shape
    shaped = source.astype(jnp.float32).reshape(sequence_count, total_row_count // BLOCK, BLOCK, local_head_count, HEAD_WIDTH)
    return shaped.transpose(0, 3, 1, 2, 4)

def block_terms(queries, keys, values, decay_logarithm, local_head_count):
    scaled_query = to_blocks(queries, local_head_count) * HEAD_WIDTH ** (-0.5)
    key_blocks = to_blocks(keys, local_head_count)
    value_blocks = to_blocks(values, local_head_count)
    decay_sum = jnp.cumsum(to_blocks(decay_logarithm, local_head_count), axis=3)
    final_log = decay_sum[:, :, :, -1:, :]
    middle = decay_sum[:, :, :, BLOCK // 2 - 1:BLOCK // 2, :]
    scores = jnp.einsum('bhncd,bhnsd->bhncs', scaled_query * jnp.exp(decay_sum - middle), key_blocks * jnp.exp(middle - decay_sum), precision=highest)
    causal = jnp.tril(jnp.ones((BLOCK, BLOCK), dtype=bool))
    scores = jnp.where(causal, scores, 0.0)
    within = jnp.einsum('bhncs,bhnse->bhnce', scores, value_blocks, precision=highest)
    block_states = jnp.einsum('bhncd,bhnce->bhnde', key_blocks * jnp.exp(final_log - decay_sum), value_blocks, precision=highest)
    return (scaled_query, decay_sum, within, block_states)

def finish(scaled_query, decay_sum, within, prior_states, outgate, head_norm_gain):
    carried = jnp.einsum('bhncd,bhnde->bhnce', scaled_query * jnp.exp(decay_sum), prior_states, precision=highest)
    merged = within + carried
    merged = merged * lax.rsqrt(lax.optimization_barrier(jnp.mean(merged * merged, axis=-1, keepdims=True)) + norm_eps)
    sequence_count, local_head_count, blocks, _, _ = merged.shape
    merged = merged.transpose(0, 2, 3, 1, 4).reshape(sequence_count, blocks * BLOCK, local_head_count * HEAD_WIDTH) * head_norm_gain
    return (merged * jax.nn.silu(outgate.astype(jnp.float32))).astype(jnp.bfloat16)

def reference(activations, input_norm_gain, pooling_channel_weight, query_projection_weight, key_projection_weight, value_projection_weight, output_gate_weight, decay_first_factor, decay_second_factor, decay_gate_bias, decay_extra_log, head_norm_gain, starting_state, pooling_group_weight, pooling_channel_scale, pooling_output_rows, attention_output_rows):
    sequence_count, length_all, model_width = activations.shape
    flat_rows = activations.reshape(sequence_count * length_all, model_width).astype(jnp.float32)
    inverse = lax.rsqrt(lax.optimization_barrier(jnp.mean(flat_rows * flat_rows, axis=1, keepdims=True)) + norm_eps)
    scaled = (flat_rows * input_norm_gain).astype(jnp.bfloat16)

    def apply_projection(weight):
        product = jnp.dot(scaled, weight, preferred_element_type=jnp.float32)
        return (product * inverse).astype(jnp.bfloat16).reshape(sequence_count, length_all, weight.shape[1])
    pool_out = pool_reference(apply_projection(pooling_channel_weight), pooling_group_weight, pooling_channel_scale)
    queries = apply_projection(query_projection_weight)
    keys = apply_projection(key_projection_weight)
    values = apply_projection(value_projection_weight)
    outgate = apply_projection(output_gate_weight)
    decay_logarithm = decay_log_values(apply_projection(decay_first_factor), decay_second_factor, decay_gate_bias, decay_extra_log)
    local_head_count = starting_state.shape[1]
    scaled_query, decay_sum, within, block_states = block_terms(queries, keys, values, decay_logarithm, local_head_count)
    block_decay = jnp.exp(decay_sum[:, :, :, -1, :])

    def advance(state_now, block_pair):
        return (block_pair[1][..., None] * state_now + block_pair[0], state_now)
    _, prior_states = lax.scan(advance, starting_state, (block_states.transpose(2, 0, 1, 3, 4), block_decay.transpose(2, 0, 1, 3)))
    prior_states = prior_states.transpose(1, 2, 0, 3, 4)
    state_out = finish(scaled_query, decay_sum, within, prior_states, outgate, head_norm_gain)
    rows_all = sequence_count * length_all
    projected = jnp.dot(pool_out.reshape(rows_all, -1), pooling_output_rows, preferred_element_type=jnp.float32)
    projected = projected + jnp.dot(state_out.reshape(rows_all, -1), attention_output_rows, preferred_element_type=jnp.float32)
    return projected.astype(jnp.bfloat16).reshape(sequence_count, length_all, model_width)
```

```python
import jax
import jax.numpy as jnp
from jax import lax
from jax.sharding import PartitionSpec as P

POOL_GROUP_WIDTH = 128
HEAD_WIDTH = 64
BLOCK = 64
REACH = 15


norm_eps = 1e-06
decay_temper = 16.0


def partner(index, step, count):
    if count & (count - 1) == 0:
        return index ^ step
    return (step - index) % count


def swap(block, axis, step):
    peers = lax.axis_size(axis)
    return lax.ppermute(block, axis, [(i, partner(i, step, peers)) for i in range(peers)])


def shifted(shard, axis, by):
    peers = lax.axis_size(axis)
    pairs = [(i, i + by) for i in range(peers) if 0 <= i + by < peers]
    return lax.ppermute(shard, axis, pairs)


def after(value, *others):
    return lax.optimization_barrier((value, *others))[0]


def line_gather(block, axis):
    peers = lax.axis_size(axis)
    own = lax.axis_index(axis)
    rightward, leftward = [block], [block]
    for _ in range(1, peers):
        rightward.append(shifted(rightward[-1], axis, 1))
        leftward.append(shifted(leftward[-1], axis, -1))
    return [block] + [
        jnp.where(own + j < peers, leftward[j], rightward[peers - j]) for j in range(1, peers)
    ]


def columns_of(array, index, count):
    width = array.shape[1] // count
    return lax.dynamic_slice_in_dim(array, index * width, width, 1)


def window_levels(extended, total_row_count):
    width_two = extended[:, 1:] + extended[:, :-1]
    width_four = width_two[:, 2:] + width_two[:, :-2]
    width_eight = width_four[:, 4:] + width_four[:, :-4]
    width_sixteen = width_eight[:, 8:] + width_eight[:, :-8]
    return (
        width_two[:, -total_row_count:],
        width_four[:, -total_row_count:],
        width_eight[:, -total_row_count:],
        width_sixteen,
    )


def pool_branch(
    pool_input, previous, pooling_group_weight, pooling_channel_scale, channel_first, position_first
):
    batch_groups, total_row_count, channels = pool_input.shape
    current = pool_input.astype(jnp.float32)
    extended = jnp.concatenate([previous.astype(jnp.float32), current], axis=1)
    window_sums = window_levels(extended, total_row_count)
    level_ids = (channel_first + jnp.arange(channels)) // POOL_GROUP_WIDTH % 4
    window = jnp.where(
        level_ids == 0, 2.0, jnp.where(level_ids == 1, 4.0, jnp.where(level_ids == 2, 8.0, 16.0))
    ).astype(jnp.float32)
    chosen = jnp.where(
        level_ids == 0,
        window_sums[0],
        jnp.where(
            level_ids == 1,
            window_sums[1],
            jnp.where(level_ids == 2, window_sums[2], window_sums[3]),
        ),
    )
    positions = (position_first + jnp.arange(total_row_count)).astype(jnp.float32)
    counts = jnp.minimum(positions[:, None] + 1.0, window[None, :])
    deviation = (chosen / counts - current).astype(jnp.bfloat16)
    grouped = deviation.reshape(
        batch_groups, total_row_count, channels // POOL_GROUP_WIDTH, POOL_GROUP_WIDTH
    )
    mixture = jnp.einsum(
        "btgc,gcd->btgd", grouped, pooling_group_weight, preferred_element_type=jnp.float32
    )
    return (
        mixture.reshape(batch_groups, total_row_count, channels) * pooling_channel_scale
    ).astype(jnp.bfloat16)


def decay_log_values(decay_lower_bound, decay_second_factor, decay_gate_bias, decay_extra_log):
    batch_groups, total_row_count, rank_width = decay_lower_bound.shape
    gate_input = (
        jnp.dot(
            decay_lower_bound.reshape(batch_groups * total_row_count, rank_width),
            decay_second_factor,
            preferred_element_type=jnp.float32,
        )
        + decay_gate_bias
    )
    logarithm_rates = jax.nn.log_sigmoid(gate_input) / decay_temper
    local_head_count = decay_extra_log.shape[0]
    logarithm_rates = (
        logarithm_rates.reshape(batch_groups, total_row_count, local_head_count, HEAD_WIDTH)
        + decay_extra_log.T[None, :, :, None]
    )
    return logarithm_rates.reshape(batch_groups, total_row_count, local_head_count * HEAD_WIDTH)


def to_blocks(source, local_head_count):
    batch_groups, total_row_count, _ = source.shape
    shaped = source.astype(jnp.float32).reshape(
        batch_groups, total_row_count // BLOCK, BLOCK, local_head_count, HEAD_WIDTH
    )
    return shaped.transpose(0, 3, 1, 2, 4)


def block_terms(queries, keys, values, decay_logarithm, local_head_count):
    scaled_query = to_blocks(queries, local_head_count) * HEAD_WIDTH ** (-0.5)
    key_blocks = to_blocks(keys, local_head_count)
    value_blocks = to_blocks(values, local_head_count)
    lower = jnp.tril(jnp.ones((BLOCK, BLOCK), jnp.float32))
    decay_sum = jnp.einsum(
        "cs,bhnsd->bhncd",
        lower,
        to_blocks(decay_logarithm, local_head_count),
        precision=lax.Precision.HIGHEST,
    )
    final_log = decay_sum[:, :, :, -1:, :]
    middle = decay_sum[:, :, :, BLOCK // 2 - 1 : BLOCK // 2, :]
    scores = jnp.einsum(
        "bhncd,bhnsd->bhncs",
        (scaled_query * jnp.exp(decay_sum - middle)).astype(jnp.bfloat16),
        (key_blocks * jnp.exp(middle - decay_sum)).astype(jnp.bfloat16),
        preferred_element_type=jnp.float32,
    )
    causal = jnp.tril(jnp.ones((BLOCK, BLOCK), dtype=bool))
    scores = jnp.where(causal, scores, 0.0)
    within = jnp.einsum("bhncs,bhnse->bhnce",
        scores.astype(jnp.bfloat16),
        value_blocks.astype(jnp.bfloat16),
        preferred_element_type=jnp.float32,
    )
    block_states = jnp.einsum(
        "bhncd,bhnce->bhnde",
        (key_blocks * jnp.exp(final_log - decay_sum)).astype(jnp.bfloat16),
        value_blocks.astype(jnp.bfloat16),
        preferred_element_type=jnp.float32,
    )
    return (scaled_query, decay_sum, within, block_states)


def finish(scaled_query, decay_sum, within, prior_states, outgate, head_norm_gain):
    carried = jnp.einsum(
        "bhncd,bhnde->bhnce",
        (scaled_query * jnp.exp(decay_sum)).astype(jnp.bfloat16),
        prior_states.astype(jnp.bfloat16),
        preferred_element_type=jnp.float32,
    )
    merged = within + carried
    merged = merged * lax.rsqrt(jnp.mean(merged * merged, axis=-1, keepdims=True) + norm_eps)
    batch_groups, local_head_count, blocks, _, _ = merged.shape
    merged = (
        merged.transpose(0, 2, 3, 1, 4).reshape(
            batch_groups, blocks * BLOCK, local_head_count * HEAD_WIDTH
        )
        * head_norm_gain
    )
    return (merged * jax.nn.silu(outgate.astype(jnp.float32))).astype(jnp.bfloat16)


def spread_body(
    activations,
    input_norm_gain,
    pooling_channel_weight,
    query_projection_weight,
    key_projection_weight,
    value_projection_weight,
    output_gate_weight,
    decay_first_factor,
    decay_second_factor,
    decay_gate_bias,
    decay_extra_log,
    head_norm_gain,
    starting_state,
    pooling_group_weight,
    pooling_channel_scale,
    pooling_output_rows,
    attention_output_rows,
):
    sequences, rows, model_width = activations.shape
    ns, nf, nt = lax.axis_size("sp"), lax.axis_size("fs"), lax.axis_size("tp")
    s, f, t = lax.axis_index("sp"), lax.axis_index("fs"), lax.axis_index("tp")
    total = nf * sequences

    output_rows = jnp.stack((pooling_output_rows, attention_output_rows))
    out_width = output_rows.shape[2] // nf
    own_quarter = lax.dynamic_slice_in_dim(output_rows, f * out_width, out_width, 2)
    row_blocks = line_gather(own_quarter, "sp")

    weights = (
        pooling_channel_weight,
        query_projection_weight,
        key_projection_weight,
        value_projection_weight,
        output_gate_weight,
    )

    def packed_for(target):
        return jnp.concatenate(
            [columns_of(w, target, nf) for w in weights] + [decay_first_factor], axis=1
        )

    packed = [packed_for(f)] + [swap(packed_for(partner(f, k, nf)), "fs", k) for k in range(1, nf)]
    depth = decay_first_factor.shape[0]
    weight_block = jnp.zeros((nf * depth, packed[0].shape[1]), jnp.bfloat16)
    for k in range(nf):
        weight_block = lax.dynamic_update_slice_in_dim(
            weight_block, packed[k], partner(f, k, nf) * depth, 0
        )
    weight_blocks = line_gather(weight_block, "sp")

    flat_rows = activations.reshape(sequences * rows, model_width).astype(jnp.float32)
    inverse = lax.rsqrt(jnp.mean(flat_rows * flat_rows, axis=1, keepdims=True) + norm_eps)
    scaled = (flat_rows * input_norm_gain).astype(jnp.bfloat16)
    flat = sequences * rows
    x_all = jnp.zeros((nf * flat, model_width), jnp.bfloat16)
    inverse_all = jnp.zeros((nf * flat, 1), jnp.float32)
    x_all = lax.dynamic_update_slice_in_dim(x_all, scaled, f * flat, 0)
    inverse_all = lax.dynamic_update_slice_in_dim(inverse_all, inverse, f * flat, 0)
    part_width = model_width // nt
    part = after(columns_of(scaled, t, nt), *packed[1:])
    for k in range(1, nf):
        source = partner(f, k, nf)
        arrived = swap(part, "fs", k)
        inverse_all = lax.dynamic_update_slice_in_dim(
            inverse_all, swap(inverse.T, "fs", k).T, source * flat, 0
        )
        x_all = lax.dynamic_update_slice(x_all, arrived, (source * flat, t * part_width))
        for m in range(1, nt):
            x_all = lax.dynamic_update_slice(
                x_all, swap(arrived, "tp", m), (source * flat, partner(t, m, nt) * part_width)
            )

    row_stack = [None] * nf
    moved = [after(b, x_all) for b in row_blocks[1:]]
    for k in range(nf):
        quarter = partner(f, k, nf)
        blocks = jnp.zeros((2, ns) + own_quarter.shape[1:], jnp.bfloat16)
        own = lax.dynamic_slice_in_dim(output_rows, quarter * out_width, out_width, 2)
        blocks = lax.dynamic_update_slice_in_dim(blocks, own[:, None], s, 1)
        for j in range(1, ns):
            arrived = moved[j - 1] if k == 0 else swap(moved[j - 1], "fs", k)
            blocks = lax.dynamic_update_slice_in_dim(blocks, arrived[:, None], (s + j) % ns, 1)
        row_stack[k] = blocks.reshape(-1, out_width)

    block_depth = nf * depth
    projected = 0.0
    for j in range(ns):
        columns = lax.dynamic_slice_in_dim(x_all, (s + j) % ns * block_depth, block_depth, 1)
        projected += jnp.dot(columns, weight_blocks[j], preferred_element_type=jnp.float32)
    projected = (projected * inverse_all).astype(jnp.bfloat16)
    sizes = [w.shape[1] // nf for w in weights] + [decay_first_factor.shape[1]]
    split_parts = []
    first = 0
    for size in sizes:
        split_parts.append(projected[:, first : first + size].reshape(total, rows, size))
        first += size
    pool_input, queries, keys, values, outgate, decay_lower_bound = split_parts

    def mine(array, axis=0):
        width = array.shape[axis] // nf
        return lax.dynamic_slice_in_dim(array, f * width, width, axis)

    head_count = starting_state.shape[1] // nf
    opening_state = jnp.zeros((total, head_count) + starting_state.shape[2:], jnp.float32)
    for k in range(nf):
        other = partner(f, k, nf)
        piece = lax.dynamic_slice_in_dim(starting_state, other * head_count, head_count, 1)
        piece = piece if k == 0 else swap(piece, "fs", k)
        opening_state = lax.dynamic_update_slice_in_dim(opening_state, piece, other * sequences, 0)
    decay_logarithm = decay_log_values(
        decay_lower_bound, mine(decay_second_factor, 1), mine(decay_gate_bias), mine(decay_extra_log)
    )
    scaled_query, decay_sum, within, block_states = block_terms(
        queries, keys, values, decay_logarithm, head_count
    )
    block_log = decay_sum[:, :, :, -1, :]
    block_decay = jnp.exp(block_log)[..., None]
    blocks = block_log.shape[2]
    state = jnp.zeros_like(opening_state)
    local_prior = []
    for n in range(blocks):
        local_prior.append(state)
        state = block_decay[:, :, n] * state + block_states[:, :, n]
    device_decay = jnp.exp(jnp.sum(block_log, axis=2))[..., None]
    bundle = jnp.concatenate((state, jnp.swapaxes(device_decay, 2, 3)), axis=2)
    incoming = opening_state
    arrivals = [shifted(bundle, "sp", k) for k in range(1, ns)]
    for k in range(ns - 1, 0, -1):
        earlier = arrivals[k - 1]
        folded = jnp.swapaxes(earlier[:, :, -1:], 2, 3) * incoming + earlier[:, :, :-1]
        incoming = jnp.where(s >= k, folded, incoming)
    opening = jnp.exp(jnp.cumsum(block_log, axis=2) - block_log)
    prior_states = jnp.stack(local_prior, axis=2) + opening[..., None] * incoming[:, :, None]
    state_out = finish(
        scaled_query, decay_sum, within, prior_states, outgate, mine(head_norm_gain)
    )

    previous = shifted(pool_input[:, rows - REACH :, :], "sp", 1)
    channels_here = pool_input.shape[2]
    pool_out = pool_branch(
        pool_input,
        previous,
        mine(pooling_group_weight),
        mine(pooling_channel_scale),
        (t * nf + f) * channels_here,
        s * rows,
    )

    feats = jnp.stack((pool_out, state_out)).reshape(2, nf, flat, channels_here)
    gathered = jnp.zeros((flat, 2, nt, nf, channels_here), jnp.bfloat16)
    for k in range(nf):
        other = partner(f, k, nf)
        piece = lax.dynamic_index_in_dim(feats, other, 1, keepdims=False)
        piece = piece if k == 0 else swap(piece, "fs", k)
        for m in range(nt):
            here = piece if m == 0 else swap(piece, "tp", m)
            gathered = lax.dynamic_update_slice(
                gathered,
                here.transpose(1, 0, 2)[:, :, None, None],
                (0, 0, partner(t, m, nt), other, 0),
            )
    gathered = gathered.reshape(flat, -1)
    result = jnp.zeros((flat, nf * out_width), jnp.bfloat16)
    for k in range(nf):
        product = jnp.dot(gathered, row_stack[k], preferred_element_type=jnp.float32)
        result = lax.dynamic_update_slice_in_dim(
            result, product.astype(jnp.bfloat16), partner(f, k, nf) * out_width, 1
        )
    return result.reshape(sequences, rows, -1)


def combine_states(earlier, later):
    return (earlier[0] * later[0], later[0][..., None] * earlier[1] + later[1])


def wide_body(
    activations,
    input_norm_gain,
    pooling_channel_weight,
    query_projection_weight,
    key_projection_weight,
    value_projection_weight,
    output_gate_weight,
    decay_first_factor,
    decay_second_factor,
    decay_gate_bias,
    decay_extra_log,
    head_norm_gain,
    starting_state,
    pooling_group_weight,
    pooling_channel_scale,
    pooling_output_rows,
    attention_output_rows,
):
    batch_groups, total_row_count, model_width = activations.shape
    flat_rows = activations.reshape(batch_groups * total_row_count, model_width).astype(jnp.float32)
    inverse = lax.rsqrt(jnp.mean(flat_rows * flat_rows, axis=1, keepdims=True) + norm_eps)
    scaled = (flat_rows * input_norm_gain).astype(jnp.bfloat16)
    column_sizes = [
        pooling_channel_weight.shape[1],
        query_projection_weight.shape[1],
        key_projection_weight.shape[1],
        value_projection_weight.shape[1],
        output_gate_weight.shape[1],
        decay_first_factor.shape[1],
    ]
    projected = jnp.dot(
        scaled,
        jnp.concatenate(
            (
                lax.all_gather(pooling_channel_weight, ("sp", "fs"), axis=0, tiled=True),
                lax.all_gather(query_projection_weight, ("sp", "fs"), axis=0, tiled=True),
                lax.all_gather(key_projection_weight, ("sp", "fs"), axis=0, tiled=True),
                lax.all_gather(value_projection_weight, ("sp", "fs"), axis=0, tiled=True),
                lax.all_gather(output_gate_weight, ("sp", "fs"), axis=0, tiled=True),
                lax.all_gather(decay_first_factor, ("sp", "fs"), axis=0, tiled=True),
            ),
            axis=1,
        ),
        preferred_element_type=jnp.float32,
    )
    projected = (projected * inverse).astype(jnp.bfloat16)
    split_parts = []
    column_first = 0
    for size_here in column_sizes:
        split_parts.append(
            projected[:, column_first : column_first + size_here].reshape(
                batch_groups, total_row_count, size_here
            )
        )
        column_first += size_here
    pool_input, queries, keys, values, outgate, decay_lower_bound = split_parts
    previous = shifted(pool_input[:, total_row_count - REACH :, :], "sp", 1)
    channels_here = pool_input.shape[2]
    pool_out = pool_branch(
        pool_input,
        previous,
        pooling_group_weight,
        pooling_channel_scale,
        lax.axis_index("tp") * channels_here,
        lax.axis_index("sp") * total_row_count,
    )
    decay_logarithm = decay_log_values(
        decay_lower_bound, decay_second_factor, decay_gate_bias, decay_extra_log
    )
    local_head_count = starting_state.shape[1]
    scaled_query, decay_sum, within, block_states = block_terms(
        queries, keys, values, decay_logarithm, local_head_count
    )
    block_log = decay_sum[:, :, :, -1, :]
    block_decay = jnp.exp(block_log)

    def advance(state_now, block_pair):
        return (block_pair[1][..., None] * state_now + block_pair[0], state_now)

    zero_state = jnp.zeros(starting_state.shape, jnp.float32)
    device_state, local_prior = lax.scan(
        advance,
        zero_state,
        (block_states.transpose(2, 0, 1, 3, 4), block_decay.transpose(2, 0, 1, 3)),
    )
    local_prior = local_prior.transpose(1, 2, 0, 3, 4)
    device_decay = jnp.exp(jnp.sum(block_log, axis=2))
    all_decay, all_state = (
        lax.all_gather(device_decay[None], "sp", axis=0, tiled=True),
        lax.all_gather(device_state[None], "sp", axis=0, tiled=True),
    )
    own_index = lax.axis_index("sp")

    def absorb(position, running_pair):
        folded = combine_states(running_pair, (all_decay[position], all_state[position]))
        keep = position < own_index
        return (
            jnp.where(keep, folded[0], running_pair[0]),
            jnp.where(keep, folded[1], running_pair[1]),
        )

    before_decay, before_state = lax.fori_loop(
        0, all_decay.shape[0], absorb, (jnp.ones_like(device_decay), jnp.zeros_like(device_state))
    )
    incoming = before_decay[..., None] * starting_state + before_state
    opening = jnp.exp(jnp.cumsum(block_log, axis=2) - block_log)
    prior_states = local_prior + opening[..., None] * incoming[:, :, None]
    state_out = finish(scaled_query, decay_sum, within, prior_states, outgate, head_norm_gain)
    pool_rows_all, state_rows_all = (
        lax.all_gather(pooling_output_rows, "sp", axis=0, tiled=True),
        lax.all_gather(attention_output_rows, "sp", axis=0, tiled=True),
    )
    accumulated = jnp.einsum(
        "btc,cd->btd",
        lax.all_gather(pool_out, "tp", axis=2, tiled=True),
        pool_rows_all,
        preferred_element_type=jnp.float32,
    )
    result = accumulated + jnp.einsum(
        "btc,cd->btd",
        lax.all_gather(state_out, "tp", axis=2, tiled=True),
        state_rows_all,
        preferred_element_type=jnp.float32,
    )
    return result.astype(jnp.bfloat16)


def body(*arrays):
    nf = lax.axis_size("fs")
    heads, groups = arrays[12].shape[1], arrays[13].shape[0]
    divisible = heads % nf == 0 and groups % nf == 0
    return (spread_body if divisible else wide_body)(*arrays)


def solution(mesh):
    in_specs = (
        P("fs", "sp", None),
        P(),
        P(("sp", "fs"), "tp"),
        P(("sp", "fs"), "tp"),
        P(("sp", "fs"), "tp"),
        P(("sp", "fs"), "tp"),
        P(("sp", "fs"), "tp"),
        P(("sp", "fs"), None),
        P(None, "tp"),
        P("tp"),
        P("tp", "sp"),
        P("tp"),
        P("fs", "tp", None, None),
        P("tp", None, None),
        P("tp"),
        P("sp", "tp"),
        P("sp", "tp"),
    )
    out_specs = P("fs", "sp", "tp")
    return jax.shard_map(body, mesh=mesh, in_specs=in_specs, out_specs=out_specs, check_vma=False)
```

```python
import jax
import jax.numpy as jnp
from jax import lax
from jax.experimental import pallas as pl
from jax.experimental.pallas import tpu as pltpu
from jax.sharding import PartitionSpec as P

POOL_GROUP_WIDTH = 128
HEAD_WIDTH = 64
BLOCK = 64
REACH = 15


norm_eps = 1e-06
decay_temper = 16.0


def partner(index, step, count):
    if count & (count - 1) == 0:
        return index ^ step
    return (step - index) % count


def swap(block, axis, step):
    peers = lax.axis_size(axis)
    return lax.ppermute(block, axis, [(i, partner(i, step, peers)) for i in range(peers)])


def shifted(shard, axis, by):
    peers = lax.axis_size(axis)
    pairs = [(i, i + by) for i in range(peers) if 0 <= i + by < peers]
    return lax.ppermute(shard, axis, pairs)


def after(value, *others):
    return lax.optimization_barrier((value, *others))[0]


def line_gather(block, axis):
    peers = lax.axis_size(axis)
    own = lax.axis_index(axis)
    rightward, leftward = [block], [block]
    for _ in range(1, peers):
        rightward.append(shifted(rightward[-1], axis, 1))
        leftward.append(shifted(leftward[-1], axis, -1))
    return [block] + [
        jnp.where(own + j < peers, leftward[j], rightward[peers - j]) for j in range(1, peers)
    ]


def pack_columns(weights, shared, index, count):
    depth, width = weights[0].shape[0], weights[0].shape[1] // count
    total = width * len(weights) + shared.shape[1]

    def kernel(index_ref, *refs):
        sources, shared_ref, targets = refs[: len(weights)], refs[len(weights)], refs[-count:]
        for k, target in enumerate(targets):
            start = pl.multiple_of(partner(index_ref[0], k, count) * width, width)
            for i, source in enumerate(sources):
                target[:, i * width : (i + 1) * width] = source[:, pl.ds(start, width)]
            target[:, len(weights) * width :] = shared_ref[...]

    return pl.pallas_call(
        kernel,
        out_shape=[jax.ShapeDtypeStruct((depth, total), shared.dtype)] * count,
        in_specs=[pl.BlockSpec(memory_space=pltpu.SMEM)]
        + [pl.BlockSpec(memory_space=pltpu.VMEM)] * (len(weights) + 1),
        out_specs=[pl.BlockSpec(memory_space=pltpu.VMEM)] * count,
    )(index.reshape(1), *weights, shared)


def place_rows(blocks, index):
    count, depth = len(blocks), blocks[0].shape[0]

    def kernel(index_ref, *refs):
        for k, source in enumerate(refs[:count]):
            start = pl.multiple_of(partner(index_ref[0], k, count) * depth, depth)
            refs[count][pl.ds(start, depth), :] = source[...]

    return pl.pallas_call(
        kernel,
        out_shape=jax.ShapeDtypeStruct((count * depth, blocks[0].shape[1]), blocks[0].dtype),
        in_specs=[pl.BlockSpec(memory_space=pltpu.SMEM)]
        + [pl.BlockSpec(memory_space=pltpu.VMEM)] * count,
        out_specs=pl.BlockSpec(memory_space=pltpu.VMEM),
    )(index.reshape(1), *blocks)


def window_levels(extended, total_row_count):
    width_two = extended[:, 1:] + extended[:, :-1]
    width_four = width_two[:, 2:] + width_two[:, :-2]
    width_eight = width_four[:, 4:] + width_four[:, :-4]
    width_sixteen = width_eight[:, 8:] + width_eight[:, :-8]
    return (
        width_two[:, -total_row_count:],
        width_four[:, -total_row_count:],
        width_eight[:, -total_row_count:],
        width_sixteen,
    )


def pool_branch(
    pool_input, previous, pooling_group_weight, pooling_channel_scale, channel_first, position_first
):
    batch_groups, total_row_count, channels = pool_input.shape
    current = pool_input.astype(jnp.float32)
    extended = jnp.concatenate([previous.astype(jnp.float32), current], axis=1)
    window_sums = window_levels(extended, total_row_count)
    level_ids = (channel_first + jnp.arange(channels)) // POOL_GROUP_WIDTH % 4
    window = jnp.where(
        level_ids == 0, 2.0, jnp.where(level_ids == 1, 4.0, jnp.where(level_ids == 2, 8.0, 16.0))
    ).astype(jnp.float32)
    chosen = jnp.where(
        level_ids == 0,
        window_sums[0],
        jnp.where(
            level_ids == 1,
            window_sums[1],
            jnp.where(level_ids == 2, window_sums[2], window_sums[3]),
        ),
    )
    positions = (position_first + jnp.arange(total_row_count)).astype(jnp.float32)
    counts = jnp.minimum(positions[:, None] + 1.0, window[None, :])
    deviation = (chosen / counts - current).astype(jnp.bfloat16)
    grouped = deviation.reshape(
        batch_groups, total_row_count, channels // POOL_GROUP_WIDTH, POOL_GROUP_WIDTH
    )
    mixture = jnp.einsum(
        "btgc,gcd->btgd", grouped, pooling_group_weight, preferred_element_type=jnp.float32
    )
    return (
        mixture.reshape(batch_groups, total_row_count, channels) * pooling_channel_scale
    ).astype(jnp.bfloat16)


def decay_log_values(decay_lower_bound, decay_second_factor, decay_gate_bias, decay_extra_log):
    batch_groups, total_row_count, rank_width = decay_lower_bound.shape
    gate_input = (
        jnp.dot(
            decay_lower_bound.reshape(batch_groups * total_row_count, rank_width),
            decay_second_factor,
            preferred_element_type=jnp.float32,
        )
        + decay_gate_bias
    )
    logarithm_rates = jax.nn.log_sigmoid(gate_input) / decay_temper
    local_head_count = decay_extra_log.shape[0]
    logarithm_rates = (
        logarithm_rates.reshape(batch_groups, total_row_count, local_head_count, HEAD_WIDTH)
        + decay_extra_log.T[None, :, :, None]
    )
    return logarithm_rates.reshape(batch_groups, total_row_count, local_head_count * HEAD_WIDTH)


def to_blocks(source, local_head_count):
    batch_groups, total_row_count, _ = source.shape
    shaped = source.astype(jnp.float32).reshape(
        batch_groups, total_row_count // BLOCK, BLOCK, local_head_count, HEAD_WIDTH
    )
    return shaped.transpose(0, 3, 1, 2, 4)


def block_terms(queries, keys, values, decay_logarithm, local_head_count):
    scaled_query = to_blocks(queries, local_head_count) * HEAD_WIDTH ** (-0.5)
    key_blocks = to_blocks(keys, local_head_count)
    value_blocks = to_blocks(values, local_head_count)
    lower = jnp.tril(jnp.ones((BLOCK, BLOCK), jnp.float32))
    decay_sum = jnp.einsum(
        "cs,bhnsd->bhncd",
        lower,
        to_blocks(decay_logarithm, local_head_count),
        precision=lax.Precision.HIGHEST,
    )
    final_log = decay_sum[:, :, :, -1:, :]
    middle = decay_sum[:, :, :, BLOCK // 2 - 1 : BLOCK // 2, :]
    scores = jnp.einsum(
        "bhncd,bhnsd->bhncs",
        (scaled_query * jnp.exp(decay_sum - middle)).astype(jnp.bfloat16),
        (key_blocks * jnp.exp(middle - decay_sum)).astype(jnp.bfloat16),
        preferred_element_type=jnp.float32,
    )
    causal = jnp.tril(jnp.ones((BLOCK, BLOCK), dtype=bool))
    scores = jnp.where(causal, scores, 0.0)
    within = jnp.einsum("bhncs,bhnse->bhnce",
        scores.astype(jnp.bfloat16),
        value_blocks.astype(jnp.bfloat16),
        preferred_element_type=jnp.float32,
    )
    block_states = jnp.einsum(
        "bhncd,bhnce->bhnde",
        (key_blocks * jnp.exp(final_log - decay_sum)).astype(jnp.bfloat16),
        value_blocks.astype(jnp.bfloat16),
        preferred_element_type=jnp.float32,
    )
    return (scaled_query, decay_sum, within, block_states)


def finish(scaled_query, decay_sum, within, prior_states, outgate, head_norm_gain):
    carried = jnp.einsum(
        "bhncd,bhnde->bhnce",
        (scaled_query * jnp.exp(decay_sum)).astype(jnp.bfloat16),
        prior_states.astype(jnp.bfloat16),
        preferred_element_type=jnp.float32,
    )
    merged = within + carried
    merged = merged * lax.rsqrt(jnp.mean(merged * merged, axis=-1, keepdims=True) + norm_eps)
    batch_groups, local_head_count, blocks, _, _ = merged.shape
    merged = (
        merged.transpose(0, 2, 3, 1, 4).reshape(
            batch_groups, blocks * BLOCK, local_head_count * HEAD_WIDTH
        )
        * head_norm_gain
    )
    return (merged * jax.nn.silu(outgate.astype(jnp.float32))).astype(jnp.bfloat16)


def spread_body(
    activations,
    input_norm_gain,
    pooling_channel_weight,
    query_projection_weight,
    key_projection_weight,
    value_projection_weight,
    output_gate_weight,
    decay_first_factor,
    decay_second_factor,
    decay_gate_bias,
    decay_extra_log,
    head_norm_gain,
    starting_state,
    pooling_group_weight,
    pooling_channel_scale,
    pooling_output_rows,
    attention_output_rows,
):
    sequences, rows, model_width = activations.shape
    ns, nf, nt = lax.axis_size("sp"), lax.axis_size("fs"), lax.axis_size("tp")
    s, f, t = lax.axis_index("sp"), lax.axis_index("fs"), lax.axis_index("tp")
    total = nf * sequences

    output_rows = jnp.stack((pooling_output_rows, attention_output_rows))
    out_width = output_rows.shape[2] // nf
    own_quarter = lax.dynamic_slice_in_dim(output_rows, f * out_width, out_width, 2)
    row_blocks = line_gather(own_quarter, "sp")

    weights = (
        pooling_channel_weight,
        query_projection_weight,
        key_projection_weight,
        value_projection_weight,
        output_gate_weight,
    )

    packed = pack_columns(weights, decay_first_factor, f, nf)
    packed = [packed[0]] + [swap(packed[k], "fs", k) for k in range(1, nf)]
    depth = decay_first_factor.shape[0]
    weight_block = place_rows(packed, f)
    weight_blocks = line_gather(weight_block, "sp")

    flat_rows = activations.reshape(sequences * rows, model_width).astype(jnp.float32)
    inverse = lax.rsqrt(jnp.mean(flat_rows * flat_rows, axis=1, keepdims=True) + norm_eps)
    scaled = (flat_rows * input_norm_gain).astype(jnp.bfloat16)
    flat = sequences * rows
    block_width = model_width // ns
    scaled = scaled.reshape(flat, ns, block_width).transpose(1, 0, 2)
    x_all = jnp.zeros((ns, nf * flat, block_width), jnp.bfloat16)
    inverse_all = jnp.zeros((nf * flat, 1), jnp.float32)
    x_all = lax.dynamic_update_slice_in_dim(x_all, scaled, f * flat, 1)
    inverse_all = lax.dynamic_update_slice_in_dim(inverse_all, inverse, f * flat, 0)
    parts = ns // nt
    part = after(lax.dynamic_slice_in_dim(scaled, t * parts, parts, 0), *packed[1:])
    for k in range(1, nf):
        source = partner(f, k, nf)
        arrived = swap(part, "fs", k)
        inverse_all = lax.dynamic_update_slice_in_dim(
            inverse_all, swap(inverse.T, "fs", k).T, source * flat, 0
        )
        x_all = lax.dynamic_update_slice(x_all, arrived, (t * parts, source * flat, 0))
        for m in range(1, nt):
            x_all = lax.dynamic_update_slice(
                x_all, swap(arrived, "tp", m), (partner(t, m, nt) * parts, source * flat, 0)
            )

    row_stack = [None] * nf
    moved = [after(b, x_all) for b in row_blocks[1:]]
    for k in range(nf):
        quarter = partner(f, k, nf)
        blocks = jnp.zeros((2, ns) + own_quarter.shape[1:], jnp.bfloat16)
        own = lax.dynamic_slice_in_dim(output_rows, quarter * out_width, out_width, 2)
        blocks = lax.dynamic_update_slice_in_dim(blocks, own[:, None], s, 1)
        for j in range(1, ns):
            arrived = moved[j - 1] if k == 0 else swap(moved[j - 1], "fs", k)
            blocks = lax.dynamic_update_slice_in_dim(blocks, arrived[:, None], (s + j) % ns, 1)
        row_stack[k] = blocks.reshape(-1, out_width)

    projected = 0.0
    for j in range(ns):
        columns = lax.dynamic_index_in_dim(x_all, (s + j) % ns, 0, keepdims=False)
        projected += jnp.dot(columns, weight_blocks[j], preferred_element_type=jnp.float32)
    projected = (projected * inverse_all).astype(jnp.bfloat16)
    sizes = [w.shape[1] // nf for w in weights] + [decay_first_factor.shape[1]]
    split_parts = []
    first = 0
    for size in sizes:
        split_parts.append(projected[:, first : first + size].reshape(total, rows, size))
        first += size
    pool_input, queries, keys, values, outgate, decay_lower_bound = split_parts

    def mine(array, axis=0):
        width = array.shape[axis] // nf
        return lax.dynamic_slice_in_dim(array, f * width, width, axis)

    head_count = starting_state.shape[1] // nf
    opening_state = jnp.zeros((total, head_count) + starting_state.shape[2:], jnp.float32)
    for k in range(nf):
        other = partner(f, k, nf)
        piece = lax.dynamic_slice_in_dim(starting_state, other * head_count, head_count, 1)
        piece = piece if k == 0 else swap(piece, "fs", k)
        opening_state = lax.dynamic_update_slice_in_dim(opening_state, piece, other * sequences, 0)
    decay_logarithm = decay_log_values(
        decay_lower_bound, mine(decay_second_factor, 1), mine(decay_gate_bias), mine(decay_extra_log)
    )
    scaled_query, decay_sum, within, block_states = block_terms(
        queries, keys, values, decay_logarithm, head_count
    )
    block_log = decay_sum[:, :, :, -1, :]
    block_decay = jnp.exp(block_log)[..., None]
    blocks = block_log.shape[2]
    state = jnp.zeros_like(opening_state)
    local_prior = []
    for n in range(blocks):
        local_prior.append(state)
        state = block_decay[:, :, n] * state + block_states[:, :, n]
    device_decay = jnp.exp(jnp.sum(block_log, axis=2))[..., None]
    bundle = jnp.concatenate((state, jnp.swapaxes(device_decay, 2, 3)), axis=2)
    incoming = opening_state
    arrivals = [shifted(bundle, "sp", k) for k in range(1, ns)]
    for k in range(ns - 1, 0, -1):
        earlier = arrivals[k - 1]
        folded = jnp.swapaxes(earlier[:, :, -1:], 2, 3) * incoming + earlier[:, :, :-1]
        incoming = jnp.where(s >= k, folded, incoming)
    opening = jnp.exp(jnp.cumsum(block_log, axis=2) - block_log)
    prior_states = jnp.stack(local_prior, axis=2) + opening[..., None] * incoming[:, :, None]
    state_out = finish(
        scaled_query, decay_sum, within, prior_states, outgate, mine(head_norm_gain)
    )

    previous = shifted(pool_input[:, rows - REACH :, :], "sp", 1)
    channels_here = pool_input.shape[2]
    pool_out = pool_branch(
        pool_input,
        previous,
        mine(pooling_group_weight),
        mine(pooling_channel_scale),
        (t * nf + f) * channels_here,
        s * rows,
    )

    feats = jnp.stack((pool_out, state_out)).reshape(2, nf, flat, channels_here)
    gathered = jnp.zeros((flat, 2, nt, nf, channels_here), jnp.bfloat16)
    for k in range(nf):
        other = partner(f, k, nf)
        piece = lax.dynamic_index_in_dim(feats, other, 1, keepdims=False)
        piece = piece if k == 0 else swap(piece, "fs", k)
        for m in range(nt):
            here = piece if m == 0 else swap(piece, "tp", m)
            gathered = lax.dynamic_update_slice(
                gathered,
                here.transpose(1, 0, 2)[:, :, None, None],
                (0, 0, partner(t, m, nt), other, 0),
            )
    gathered = gathered.reshape(flat, -1)
    result = jnp.zeros((flat, nf * out_width), jnp.bfloat16)
    for k in range(nf):
        product = jnp.dot(gathered, row_stack[k], preferred_element_type=jnp.float32)
        result = lax.dynamic_update_slice_in_dim(
            result, product.astype(jnp.bfloat16), partner(f, k, nf) * out_width, 1
        )
    return result.reshape(sequences, rows, -1)


def combine_states(earlier, later):
    return (earlier[0] * later[0], later[0][..., None] * earlier[1] + later[1])


def wide_body(
    activations,
    input_norm_gain,
    pooling_channel_weight,
    query_projection_weight,
    key_projection_weight,
    value_projection_weight,
    output_gate_weight,
    decay_first_factor,
    decay_second_factor,
    decay_gate_bias,
    decay_extra_log,
    head_norm_gain,
    starting_state,
    pooling_group_weight,
    pooling_channel_scale,
    pooling_output_rows,
    attention_output_rows,
):
    batch_groups, total_row_count, model_width = activations.shape
    flat_rows = activations.reshape(batch_groups * total_row_count, model_width).astype(jnp.float32)
    inverse = lax.rsqrt(jnp.mean(flat_rows * flat_rows, axis=1, keepdims=True) + norm_eps)
    scaled = (flat_rows * input_norm_gain).astype(jnp.bfloat16)
    column_sizes = [
        pooling_channel_weight.shape[1],
        query_projection_weight.shape[1],
        key_projection_weight.shape[1],
        value_projection_weight.shape[1],
        output_gate_weight.shape[1],
        decay_first_factor.shape[1],
    ]
    projected = jnp.dot(
        scaled,
        jnp.concatenate(
            (
                lax.all_gather(pooling_channel_weight, ("sp", "fs"), axis=0, tiled=True),
                lax.all_gather(query_projection_weight, ("sp", "fs"), axis=0, tiled=True),
                lax.all_gather(key_projection_weight, ("sp", "fs"), axis=0, tiled=True),
                lax.all_gather(value_projection_weight, ("sp", "fs"), axis=0, tiled=True),
                lax.all_gather(output_gate_weight, ("sp", "fs"), axis=0, tiled=True),
                lax.all_gather(decay_first_factor, ("sp", "fs"), axis=0, tiled=True),
            ),
            axis=1,
        ),
        preferred_element_type=jnp.float32,
    )
    projected = (projected * inverse).astype(jnp.bfloat16)
    split_parts = []
    column_first = 0
    for size_here in column_sizes:
        split_parts.append(
            projected[:, column_first : column_first + size_here].reshape(
                batch_groups, total_row_count, size_here
            )
        )
        column_first += size_here
    pool_input, queries, keys, values, outgate, decay_lower_bound = split_parts
    previous = shifted(pool_input[:, total_row_count - REACH :, :], "sp", 1)
    channels_here = pool_input.shape[2]
    pool_out = pool_branch(
        pool_input,
        previous,
        pooling_group_weight,
        pooling_channel_scale,
        lax.axis_index("tp") * channels_here,
        lax.axis_index("sp") * total_row_count,
    )
    decay_logarithm = decay_log_values(
        decay_lower_bound, decay_second_factor, decay_gate_bias, decay_extra_log
    )
    local_head_count = starting_state.shape[1]
    scaled_query, decay_sum, within, block_states = block_terms(
        queries, keys, values, decay_logarithm, local_head_count
    )
    block_log = decay_sum[:, :, :, -1, :]
    block_decay = jnp.exp(block_log)

    def advance(state_now, block_pair):
        return (block_pair[1][..., None] * state_now + block_pair[0], state_now)

    zero_state = jnp.zeros(starting_state.shape, jnp.float32)
    device_state, local_prior = lax.scan(
        advance,
        zero_state,
        (block_states.transpose(2, 0, 1, 3, 4), block_decay.transpose(2, 0, 1, 3)),
    )
    local_prior = local_prior.transpose(1, 2, 0, 3, 4)
    device_decay = jnp.exp(jnp.sum(block_log, axis=2))
    all_decay, all_state = (
        lax.all_gather(device_decay[None], "sp", axis=0, tiled=True),
        lax.all_gather(device_state[None], "sp", axis=0, tiled=True),
    )
    own_index = lax.axis_index("sp")

    def absorb(position, running_pair):
        folded = combine_states(running_pair, (all_decay[position], all_state[position]))
        keep = position < own_index
        return (
            jnp.where(keep, folded[0], running_pair[0]),
            jnp.where(keep, folded[1], running_pair[1]),
        )

    before_decay, before_state = lax.fori_loop(
        0, all_decay.shape[0], absorb, (jnp.ones_like(device_decay), jnp.zeros_like(device_state))
    )
    incoming = before_decay[..., None] * starting_state + before_state
    opening = jnp.exp(jnp.cumsum(block_log, axis=2) - block_log)
    prior_states = local_prior + opening[..., None] * incoming[:, :, None]
    state_out = finish(scaled_query, decay_sum, within, prior_states, outgate, head_norm_gain)
    pool_rows_all, state_rows_all = (
        lax.all_gather(pooling_output_rows, "sp", axis=0, tiled=True),
        lax.all_gather(attention_output_rows, "sp", axis=0, tiled=True),
    )
    accumulated = jnp.einsum(
        "btc,cd->btd",
        lax.all_gather(pool_out, "tp", axis=2, tiled=True),
        pool_rows_all,
        preferred_element_type=jnp.float32,
    )
    result = accumulated + jnp.einsum(
        "btc,cd->btd",
        lax.all_gather(state_out, "tp", axis=2, tiled=True),
        state_rows_all,
        preferred_element_type=jnp.float32,
    )
    return result.astype(jnp.bfloat16)


def body(*arrays):
    nf = lax.axis_size("fs")
    heads, groups = arrays[12].shape[1], arrays[13].shape[0]
    divisible = heads % nf == 0 and groups % nf == 0
    divisible = divisible and lax.axis_size("sp") % lax.axis_size("tp") == 0
    return (spread_body if divisible else wide_body)(*arrays)


def solution(mesh):
    in_specs = (
        P("fs", "sp", None),
        P(),
        P(("sp", "fs"), "tp"),
        P(("sp", "fs"), "tp"),
        P(("sp", "fs"), "tp"),
        P(("sp", "fs"), "tp"),
        P(("sp", "fs"), "tp"),
        P(("sp", "fs"), None),
        P(None, "tp"),
        P("tp"),
        P("tp", "sp"),
        P("tp"),
        P("fs", "tp", None, None),
        P("tp", None, None),
        P("tp"),
        P("sp", "tp"),
        P("sp", "tp"),
    )
    out_specs = P("fs", "sp", "tp")
    return jax.shard_map(body, mesh=mesh, in_specs=in_specs, out_specs=out_specs, check_vma=False)
```

```python
import jax
import jax.numpy as jnp
from jax import lax
from jax.experimental import pallas as pl
from jax.experimental.pallas import tpu as pltpu
from jax.sharding import PartitionSpec as P

POOL_GROUP_WIDTH = 128
HEAD_WIDTH = 64
BLOCK = 64
REACH = 15


norm_eps = 1e-06
decay_temper = 16.0


def partner(index, step, count):
    if count & (count - 1) == 0:
        return index ^ step
    return (step - index) % count


def swap(block, axis, step):
    peers = lax.axis_size(axis)
    return lax.ppermute(block, axis, [(i, partner(i, step, peers)) for i in range(peers)])


def shifted(shard, axis, by):
    peers = lax.axis_size(axis)
    pairs = [(i, i + by) for i in range(peers) if 0 <= i + by < peers]
    return lax.ppermute(shard, axis, pairs)


def after(value, *others):
    return lax.optimization_barrier((value, *others))[0]


def line_steps(block, axis):
    peers = lax.axis_size(axis)
    from_above, from_below = [block], [block]
    for _ in range(1, peers):
        from_above.append(shifted(from_above[-1], axis, -1))
        from_below.append(shifted(from_below[-1], axis, 1))
    return from_above, from_below


def line_gather(block, axis):
    peers = lax.axis_size(axis)
    own = lax.axis_index(axis)
    from_above, from_below = line_steps(block, axis)
    return [block] + [
        jnp.where(own + j < peers, from_above[j], from_below[peers - j]) for j in range(1, peers)
    ]


def pack_columns(weights, shared, index, count):
    depth, width = weights[0].shape[0], weights[0].shape[1] // count
    total = width * len(weights) + shared.shape[1]

    def kernel(index_ref, *refs):
        sources, shared_ref, targets = refs[: len(weights)], refs[len(weights)], refs[-count:]
        for k, target in enumerate(targets):
            start = pl.multiple_of(partner(index_ref[0], k, count) * width, width)
            for i, source in enumerate(sources):
                target[:, i * width : (i + 1) * width] = source[:, pl.ds(start, width)]
            target[:, len(weights) * width :] = shared_ref[...]

    return pl.pallas_call(
        kernel,
        out_shape=[jax.ShapeDtypeStruct((depth, total), shared.dtype)] * count,
        in_specs=[pl.BlockSpec(memory_space=pltpu.SMEM)]
        + [pl.BlockSpec(memory_space=pltpu.VMEM)] * (len(weights) + 1),
        out_specs=[pl.BlockSpec(memory_space=pltpu.VMEM)] * count,
    )(index.reshape(1), *weights, shared)


def place_rows(blocks, index):
    count, depth = len(blocks), blocks[0].shape[0]

    def kernel(index_ref, *refs):
        for k, source in enumerate(refs[:count]):
            start = pl.multiple_of(partner(index_ref[0], k, count) * depth, depth)
            refs[count][pl.ds(start, depth), :] = source[...]

    return pl.pallas_call(
        kernel,
        out_shape=jax.ShapeDtypeStruct((count * depth, blocks[0].shape[1]), blocks[0].dtype),
        in_specs=[pl.BlockSpec(memory_space=pltpu.SMEM)]
        + [pl.BlockSpec(memory_space=pltpu.VMEM)] * count,
        out_specs=pl.BlockSpec(memory_space=pltpu.VMEM),
    )(index.reshape(1), *blocks)


def window_levels(extended, total_row_count):
    width_two = extended[:, 1:] + extended[:, :-1]
    width_four = width_two[:, 2:] + width_two[:, :-2]
    width_eight = width_four[:, 4:] + width_four[:, :-4]
    width_sixteen = width_eight[:, 8:] + width_eight[:, :-8]
    return (
        width_two[:, -total_row_count:],
        width_four[:, -total_row_count:],
        width_eight[:, -total_row_count:],
        width_sixteen,
    )


def pool_branch(
    pool_input, previous, pooling_group_weight, pooling_channel_scale, channel_first, position_first
):
    batch_groups, total_row_count, channels = pool_input.shape
    current = pool_input.astype(jnp.float32)
    extended = jnp.concatenate([previous.astype(jnp.float32), current], axis=1)
    window_sums = window_levels(extended, total_row_count)
    level_ids = (channel_first + jnp.arange(channels)) // POOL_GROUP_WIDTH % 4
    window = jnp.where(
        level_ids == 0, 2.0, jnp.where(level_ids == 1, 4.0, jnp.where(level_ids == 2, 8.0, 16.0))
    ).astype(jnp.float32)
    chosen = jnp.where(
        level_ids == 0,
        window_sums[0],
        jnp.where(
            level_ids == 1,
            window_sums[1],
            jnp.where(level_ids == 2, window_sums[2], window_sums[3]),
        ),
    )
    positions = (position_first + jnp.arange(total_row_count)).astype(jnp.float32)
    counts = jnp.minimum(positions[:, None] + 1.0, window[None, :])
    deviation = (chosen / counts - current).astype(jnp.bfloat16)
    grouped = deviation.reshape(
        batch_groups, total_row_count, channels // POOL_GROUP_WIDTH, POOL_GROUP_WIDTH
    )
    mixture = jnp.einsum(
        "btgc,gcd->btgd", grouped, pooling_group_weight, preferred_element_type=jnp.float32
    )
    return (
        mixture.reshape(batch_groups, total_row_count, channels) * pooling_channel_scale
    ).astype(jnp.bfloat16)


def decay_log_values(decay_lower_bound, decay_second_factor, decay_gate_bias, decay_extra_log):
    batch_groups, total_row_count, rank_width = decay_lower_bound.shape
    gate_input = (
        jnp.dot(
            decay_lower_bound.reshape(batch_groups * total_row_count, rank_width),
            decay_second_factor,
            preferred_element_type=jnp.float32,
        )
        + decay_gate_bias
    )
    logarithm_rates = jax.nn.log_sigmoid(gate_input) / decay_temper
    local_head_count = decay_extra_log.shape[0]
    logarithm_rates = (
        logarithm_rates.reshape(batch_groups, total_row_count, local_head_count, HEAD_WIDTH)
        + decay_extra_log.T[None, :, :, None]
    )
    return logarithm_rates.reshape(batch_groups, total_row_count, local_head_count * HEAD_WIDTH)


def to_blocks(source, local_head_count):
    batch_groups, total_row_count, _ = source.shape
    shaped = source.astype(jnp.float32).reshape(
        batch_groups, total_row_count // BLOCK, BLOCK, local_head_count, HEAD_WIDTH
    )
    return shaped.transpose(0, 3, 1, 2, 4)


def block_terms(queries, keys, values, decay_logarithm, local_head_count):
    scaled_query = to_blocks(queries, local_head_count) * HEAD_WIDTH ** (-0.5)
    key_blocks = to_blocks(keys, local_head_count)
    value_blocks = to_blocks(values, local_head_count)
    lower = jnp.tril(jnp.ones((BLOCK, BLOCK), jnp.float32))
    decay_sum = jnp.einsum(
        "cs,bhnsd->bhncd",
        lower,
        to_blocks(decay_logarithm, local_head_count),
        precision=lax.Precision.HIGHEST,
    )
    final_log = decay_sum[:, :, :, -1:, :]
    middle = decay_sum[:, :, :, BLOCK // 2 - 1 : BLOCK // 2, :]
    scores = jnp.einsum(
        "bhncd,bhnsd->bhncs",
        (scaled_query * jnp.exp(decay_sum - middle)).astype(jnp.bfloat16),
        (key_blocks * jnp.exp(middle - decay_sum)).astype(jnp.bfloat16),
        preferred_element_type=jnp.float32,
    )
    causal = jnp.tril(jnp.ones((BLOCK, BLOCK), dtype=bool))
    scores = jnp.where(causal, scores, 0.0)
    within = jnp.einsum("bhncs,bhnse->bhnce",
        scores.astype(jnp.bfloat16),
        value_blocks.astype(jnp.bfloat16),
        preferred_element_type=jnp.float32,
    )
    block_states = jnp.einsum(
        "bhncd,bhnce->bhnde",
        (key_blocks * jnp.exp(final_log - decay_sum)).astype(jnp.bfloat16),
        value_blocks.astype(jnp.bfloat16),
        preferred_element_type=jnp.float32,
    )
    return (scaled_query, decay_sum, within, block_states)


def finish(scaled_query, decay_sum, within, prior_states, outgate, head_norm_gain):
    carried = jnp.einsum(
        "bhncd,bhnde->bhnce",
        (scaled_query * jnp.exp(decay_sum)).astype(jnp.bfloat16),
        prior_states.astype(jnp.bfloat16),
        preferred_element_type=jnp.float32,
    )
    merged = within + carried
    merged = merged * lax.rsqrt(jnp.mean(merged * merged, axis=-1, keepdims=True) + norm_eps)
    batch_groups, local_head_count, blocks, _, _ = merged.shape
    merged = (
        merged.transpose(0, 2, 3, 1, 4).reshape(
            batch_groups, blocks * BLOCK, local_head_count * HEAD_WIDTH
        )
        * head_norm_gain
    )
    return (merged * jax.nn.silu(outgate.astype(jnp.float32))).astype(jnp.bfloat16)


def spread_body(
    activations,
    input_norm_gain,
    pooling_channel_weight,
    query_projection_weight,
    key_projection_weight,
    value_projection_weight,
    output_gate_weight,
    decay_first_factor,
    decay_second_factor,
    decay_gate_bias,
    decay_extra_log,
    head_norm_gain,
    starting_state,
    pooling_group_weight,
    pooling_channel_scale,
    pooling_output_rows,
    attention_output_rows,
):
    sequences, rows, model_width = activations.shape
    ns, nf, nt = lax.axis_size("sp"), lax.axis_size("fs"), lax.axis_size("tp")
    s, f, t = lax.axis_index("sp"), lax.axis_index("fs"), lax.axis_index("tp")
    total = nf * sequences

    output_rows = jnp.stack((pooling_output_rows, attention_output_rows))
    out_width = output_rows.shape[2] // nf
    own_quarter = lax.dynamic_slice_in_dim(output_rows, f * out_width, out_width, 2)
    row_blocks = line_gather(own_quarter, "sp")

    weights = (
        pooling_channel_weight,
        query_projection_weight,
        key_projection_weight,
        value_projection_weight,
        output_gate_weight,
    )

    packed = pack_columns(weights, decay_first_factor, f, nf)
    packed = [packed[0]] + [swap(packed[k], "fs", k) for k in range(1, nf)]
    depth = decay_first_factor.shape[0]
    weight_block = place_rows(packed, f)
    above, below = line_steps(weight_block, "sp")
    activations, starting_state = lax.optimization_barrier(
        (activations, starting_state, weight_block)
    )[:2]

    flat_rows = activations.reshape(sequences * rows, model_width).astype(jnp.float32)
    inverse = lax.rsqrt(jnp.mean(flat_rows * flat_rows, axis=1, keepdims=True) + norm_eps)
    scaled = (flat_rows * input_norm_gain).astype(jnp.bfloat16)
    flat = sequences * rows
    block_width = model_width // ns
    scaled = scaled.reshape(flat, ns, block_width).transpose(1, 0, 2)
    x_all = jnp.zeros((ns, nf * flat, block_width), jnp.bfloat16)
    inverse_all = jnp.zeros((nf * flat, 1), jnp.float32)
    x_all = lax.dynamic_update_slice_in_dim(x_all, scaled, f * flat, 1)
    inverse_all = lax.dynamic_update_slice_in_dim(inverse_all, inverse, f * flat, 0)
    parts = ns // nt
    part = after(lax.dynamic_slice_in_dim(scaled, t * parts, parts, 0), *packed[1:])
    for k in range(1, nf):
        source = partner(f, k, nf)
        arrived = swap(part, "fs", k)
        inverse_all = lax.dynamic_update_slice_in_dim(
            inverse_all, swap(inverse.T, "fs", k).T, source * flat, 0
        )
        x_all = lax.dynamic_update_slice(x_all, arrived, (t * parts, source * flat, 0))
        for m in range(1, nt):
            x_all = lax.dynamic_update_slice(
                x_all, swap(arrived, "tp", m), (partner(t, m, nt) * parts, source * flat, 0)
            )

    row_stack = [None] * nf
    gate = max(ns - 2, 0)
    moved = after(jnp.stack(row_blocks[1:]), x_all, above[gate], below[gate])
    for k in range(nf):
        quarter = partner(f, k, nf)
        blocks = jnp.zeros((2, ns) + own_quarter.shape[1:], jnp.bfloat16)
        own = lax.dynamic_slice_in_dim(output_rows, quarter * out_width, out_width, 2)
        blocks = lax.dynamic_update_slice_in_dim(blocks, own[:, None], s, 1)
        arrived = moved if k == 0 else swap(moved, "fs", k)
        for j in range(1, ns):
            blocks = lax.dynamic_update_slice_in_dim(
                blocks, arrived[j - 1][:, None], (s + j) % ns, 1
            )
        row_stack[k] = blocks.reshape(-1, out_width)

    def partial(block, source):
        columns = lax.dynamic_index_in_dim(x_all, source % ns, 0, keepdims=False)
        return jnp.dot(columns, block, preferred_element_type=jnp.float32)

    projected = partial(weight_block, s)
    for j in range(1, ns):
        if 2 * j < ns:
            projected += partial(above[j], s + j)
            projected += partial(below[j], s + ns - j)
        else:
            higher = s + j < ns
            block = jnp.where(higher, above[j], below[j])
            projected += partial(block, jnp.where(higher, s + j, s + ns - j))
    projected = (projected * inverse_all).astype(jnp.bfloat16)
    sizes = [w.shape[1] // nf for w in weights] + [decay_first_factor.shape[1]]
    split_parts = []
    first = 0
    for size in sizes:
        split_parts.append(projected[:, first : first + size].reshape(total, rows, size))
        first += size
    pool_input, queries, keys, values, outgate, decay_lower_bound = split_parts

    def mine(array, axis=0):
        width = array.shape[axis] // nf
        return lax.dynamic_slice_in_dim(array, f * width, width, axis)

    head_count = starting_state.shape[1] // nf
    opening_state = jnp.zeros((total, head_count) + starting_state.shape[2:], jnp.float32)
    for k in range(nf):
        other = partner(f, k, nf)
        piece = lax.dynamic_slice_in_dim(starting_state, other * head_count, head_count, 1)
        piece = piece if k == 0 else swap(piece, "fs", k)
        opening_state = lax.dynamic_update_slice_in_dim(opening_state, piece, other * sequences, 0)
    decay_logarithm = decay_log_values(
        decay_lower_bound, mine(decay_second_factor, 1), mine(decay_gate_bias), mine(decay_extra_log)
    )
    scaled_query, decay_sum, within, block_states = block_terms(
        queries, keys, values, decay_logarithm, head_count
    )
    block_log = decay_sum[:, :, :, -1, :]
    block_decay = jnp.exp(block_log)[..., None]
    blocks = block_log.shape[2]
    state = jnp.zeros_like(opening_state)
    local_prior = []
    for n in range(blocks):
        local_prior.append(state)
        state = block_decay[:, :, n] * state + block_states[:, :, n]
    device_decay = jnp.exp(jnp.sum(block_log, axis=2))[..., None]
    bundle = jnp.concatenate((state, jnp.swapaxes(device_decay, 2, 3)), axis=2)
    incoming = opening_state
    arrivals = [shifted(bundle, "sp", k) for k in range(1, ns)]
    for k in range(ns - 1, 0, -1):
        earlier = arrivals[k - 1]
        folded = jnp.swapaxes(earlier[:, :, -1:], 2, 3) * incoming + earlier[:, :, :-1]
        incoming = jnp.where(s >= k, folded, incoming)
    opening = jnp.exp(jnp.cumsum(block_log, axis=2) - block_log)
    prior_states = jnp.stack(local_prior, axis=2) + opening[..., None] * incoming[:, :, None]
    state_out = finish(
        scaled_query, decay_sum, within, prior_states, outgate, mine(head_norm_gain)
    )

    previous = shifted(pool_input[:, rows - REACH :, :], "sp", 1)
    channels_here = pool_input.shape[2]
    pool_out = pool_branch(
        pool_input,
        previous,
        mine(pooling_group_weight),
        mine(pooling_channel_scale),
        (t * nf + f) * channels_here,
        s * rows,
    )

    feats = jnp.stack((pool_out, state_out)).reshape(2, nf, flat, channels_here)
    gathered = jnp.zeros((flat, 2, nt, nf, channels_here), jnp.bfloat16)
    for k in range(nf):
        other = partner(f, k, nf)
        piece = lax.dynamic_index_in_dim(feats, other, 1, keepdims=False)
        piece = piece if k == 0 else swap(piece, "fs", k)
        for m in range(nt):
            here = piece if m == 0 else swap(piece, "tp", m)
            gathered = lax.dynamic_update_slice(
                gathered,
                here.transpose(1, 0, 2)[:, :, None, None],
                (0, 0, partner(t, m, nt), other, 0),
            )
    gathered = gathered.reshape(flat, -1)
    result = jnp.zeros((flat, nf * out_width), jnp.bfloat16)
    for k in range(nf):
        product = jnp.dot(gathered, row_stack[k], preferred_element_type=jnp.float32)
        result = lax.dynamic_update_slice_in_dim(
            result, product.astype(jnp.bfloat16), partner(f, k, nf) * out_width, 1
        )
    return result.reshape(sequences, rows, -1)


def combine_states(earlier, later):
    return (earlier[0] * later[0], later[0][..., None] * earlier[1] + later[1])


def wide_body(
    activations,
    input_norm_gain,
    pooling_channel_weight,
    query_projection_weight,
    key_projection_weight,
    value_projection_weight,
    output_gate_weight,
    decay_first_factor,
    decay_second_factor,
    decay_gate_bias,
    decay_extra_log,
    head_norm_gain,
    starting_state,
    pooling_group_weight,
    pooling_channel_scale,
    pooling_output_rows,
    attention_output_rows,
):
    batch_groups, total_row_count, model_width = activations.shape
    flat_rows = activations.reshape(batch_groups * total_row_count, model_width).astype(jnp.float32)
    inverse = lax.rsqrt(jnp.mean(flat_rows * flat_rows, axis=1, keepdims=True) + norm_eps)
    scaled = (flat_rows * input_norm_gain).astype(jnp.bfloat16)
    column_sizes = [
        pooling_channel_weight.shape[1],
        query_projection_weight.shape[1],
        key_projection_weight.shape[1],
        value_projection_weight.shape[1],
        output_gate_weight.shape[1],
        decay_first_factor.shape[1],
    ]
    projected = jnp.dot(
        scaled,
        jnp.concatenate(
            (
                lax.all_gather(pooling_channel_weight, ("sp", "fs"), axis=0, tiled=True),
                lax.all_gather(query_projection_weight, ("sp", "fs"), axis=0, tiled=True),
                lax.all_gather(key_projection_weight, ("sp", "fs"), axis=0, tiled=True),
                lax.all_gather(value_projection_weight, ("sp", "fs"), axis=0, tiled=True),
                lax.all_gather(output_gate_weight, ("sp", "fs"), axis=0, tiled=True),
                lax.all_gather(decay_first_factor, ("sp", "fs"), axis=0, tiled=True),
            ),
            axis=1,
        ),
        preferred_element_type=jnp.float32,
    )
    projected = (projected * inverse).astype(jnp.bfloat16)
    split_parts = []
    column_first = 0
    for size_here in column_sizes:
        split_parts.append(
            projected[:, column_first : column_first + size_here].reshape(
                batch_groups, total_row_count, size_here
            )
        )
        column_first += size_here
    pool_input, queries, keys, values, outgate, decay_lower_bound = split_parts
    previous = shifted(pool_input[:, total_row_count - REACH :, :], "sp", 1)
    channels_here = pool_input.shape[2]
    pool_out = pool_branch(
        pool_input,
        previous,
        pooling_group_weight,
        pooling_channel_scale,
        lax.axis_index("tp") * channels_here,
        lax.axis_index("sp") * total_row_count,
    )
    decay_logarithm = decay_log_values(
        decay_lower_bound, decay_second_factor, decay_gate_bias, decay_extra_log
    )
    local_head_count = starting_state.shape[1]
    scaled_query, decay_sum, within, block_states = block_terms(
        queries, keys, values, decay_logarithm, local_head_count
    )
    block_log = decay_sum[:, :, :, -1, :]
    block_decay = jnp.exp(block_log)

    def advance(state_now, block_pair):
        return (block_pair[1][..., None] * state_now + block_pair[0], state_now)

    zero_state = jnp.zeros(starting_state.shape, jnp.float32)
    device_state, local_prior = lax.scan(
        advance,
        zero_state,
        (block_states.transpose(2, 0, 1, 3, 4), block_decay.transpose(2, 0, 1, 3)),
    )
    local_prior = local_prior.transpose(1, 2, 0, 3, 4)
    device_decay = jnp.exp(jnp.sum(block_log, axis=2))
    all_decay, all_state = (
        lax.all_gather(device_decay[None], "sp", axis=0, tiled=True),
        lax.all_gather(device_state[None], "sp", axis=0, tiled=True),
    )
    own_index = lax.axis_index("sp")

    def absorb(position, running_pair):
        folded = combine_states(running_pair, (all_decay[position], all_state[position]))
        keep = position < own_index
        return (
            jnp.where(keep, folded[0], running_pair[0]),
            jnp.where(keep, folded[1], running_pair[1]),
        )

    before_decay, before_state = lax.fori_loop(
        0, all_decay.shape[0], absorb, (jnp.ones_like(device_decay), jnp.zeros_like(device_state))
    )
    incoming = before_decay[..., None] * starting_state + before_state
    opening = jnp.exp(jnp.cumsum(block_log, axis=2) - block_log)
    prior_states = local_prior + opening[..., None] * incoming[:, :, None]
    state_out = finish(scaled_query, decay_sum, within, prior_states, outgate, head_norm_gain)
    pool_rows_all, state_rows_all = (
        lax.all_gather(pooling_output_rows, "sp", axis=0, tiled=True),
        lax.all_gather(attention_output_rows, "sp", axis=0, tiled=True),
    )
    accumulated = jnp.einsum(
        "btc,cd->btd",
        lax.all_gather(pool_out, "tp", axis=2, tiled=True),
        pool_rows_all,
        preferred_element_type=jnp.float32,
    )
    result = accumulated + jnp.einsum(
        "btc,cd->btd",
        lax.all_gather(state_out, "tp", axis=2, tiled=True),
        state_rows_all,
        preferred_element_type=jnp.float32,
    )
    return result.astype(jnp.bfloat16)


def body(*arrays):
    nf = lax.axis_size("fs")
    heads, groups = arrays[12].shape[1], arrays[13].shape[0]
    divisible = heads % nf == 0 and groups % nf == 0
    divisible = divisible and lax.axis_size("sp") % lax.axis_size("tp") == 0
    return (spread_body if divisible else wide_body)(*arrays)


def solution(mesh):
    in_specs = (
        P("fs", "sp", None),
        P(),
        P(("sp", "fs"), "tp"),
        P(("sp", "fs"), "tp"),
        P(("sp", "fs"), "tp"),
        P(("sp", "fs"), "tp"),
        P(("sp", "fs"), "tp"),
        P(("sp", "fs"), None),
        P(None, "tp"),
        P("tp"),
        P("tp", "sp"),
        P("tp"),
        P("fs", "tp", None, None),
        P("tp", None, None),
        P("tp"),
        P("sp", "tp"),
        P("sp", "tp"),
    )
    out_specs = P("fs", "sp", "tp")
    return jax.shard_map(body, mesh=mesh, in_specs=in_specs, out_specs=out_specs, check_vma=False)
```
